32 devices in a mesh: dp: 4 (over y, x), kv: 4 (over z), tp: 2 (over core).
Axes of the slice: x: 2, y: 2, z: 4, core: 2. Of those that a mesh axis runs over, the one named last changes fastest.
Arguments:
- tokens: bfloat16 [16, 16, 2048], P('dp', None, 'kv'), may hold values from -6 to 6
- norm_gain: float32 [2048], P('kv'), may hold values from 0.1 to 1.9
- w_query: bfloat16 [2048, 1024], P('kv', 'tp'), may hold values from -0.125 to 0.125
- w_key: bfloat16 [2048, 1024], P('kv', 'tp'), may hold values from -0.125 to 0.125
- w_value: bfloat16 [2048, 1024], P('kv', 'tp'), may hold values from -0.125 to 0.125
- w_forget: bfloat16 [2048, 16], replicated, may hold values from -0.125 to 0.125
- forget_bias: float32 [16], replicated, may hold values from -2 to 4
- query_gain: float32 [64], replicated, may hold values from 0.1 to 1.9
- key_gain: float32 [64], replicated, may hold values from 0.1 to 1.9
- head_gain: float32 [64], replicated, may hold values from 0.1 to 1.9
- w_out: bfloat16 [1024, 2048], P('tp', 'kv'), may hold values from -0.1875 to 0.1875
- key_cache: bfloat16 [16, 2048, 1024], P('dp', 'kv', 'tp'), may hold values from -240 to 240
- value_cache: bfloat16 [16, 2048, 1024], P('dp', 'kv', 'tp'), may hold values from -6 to 6
- gate_cache: float32 [16, 16, 2048], P('dp', 'tp', 'kv'), may hold values from -242 to 0, as said below
- lengths: int32 [16], P('dp'), may hold values from 1005 to 2028
- accepted: int32 [16], P('dp'), may hold values from 0 to 4
- parents: int32 [16, 16], P('dp'), may hold values from -1 to 14, as said below
Outputs:
- layer_out: bfloat16 [16, 16, 2048], P('dp', None, 'kv')
- new_keys: bfloat16 [16, 2048, 1024], P('dp', 'kv', 'tp')
- new_values: bfloat16 [16, 2048, 1024], P('dp', 'kv', 'tp')
- proposal_gates: float32 [16, 16, 16], P('dp', None, 'tp')
The draws below stay inside these ranges and needn't reach their ends.
Inputs may be any that keep to these rules, and one draw needn't show every extreme that they name: `gate_cache`: each entry is the running sum of log forget gates up to its position, so entries never rise along positions; entries at and after lengths hold the last step's proposals in order. `parents`: proposal 0 follows the last accepted token (parent -1); every other proposal's parent is one of the three proposals before it.
All inputs are finite; a program needn't handle non-finite values.
Results may differ from the reference program's by a relative error of at most 0.0051.
The reference program's roundings to bfloat16 on the way (of `scaled`, `values_new` and `normed`) count: a program that leaves them out, or rounds other values in their place, can miss the bound.
Values may be sent and summed in bfloat16 or wider, within the bound.
A program may use at most 64 MiB of HBM per device.

```python
import jax
import jax.numpy as jnp
from jax import lax

D = 2048
HEADS = 16
DH = 64
PROPS = 16
ACCEPT_MOST = 4
POS_DEV = 512
HW = 1024
HEAD_GROUP = 8
SEQUENCE_TOTAL = 16
CACHE_POSITIONS = 2048
N_KV = 4
N_TP = 2


def draw_key_cache(key, part):
    key_one = jax.random.fold_in(key, 0)
    entries = jnp.clip(jax.random.normal(key_one, (SEQUENCE_TOTAL, CACHE_POSITIONS, HEADS * DH), jnp.float32), -6.0, 6.0)
    return entries.astype(jnp.bfloat16)


def draw_gate_cache(key, part):
    every_key = jax.random.split(key, 7)
    slow_share = 0.5
    slow_heads = jax.random.uniform(every_key[0], (SEQUENCE_TOTAL, HEADS, 1)) < slow_share
    slow_rate = jax.random.uniform(every_key[1], (SEQUENCE_TOTAL, HEADS, 1), minval=0.2, maxval=0.8) / CACHE_POSITIONS
    fast_rate = 1.0 / (POS_DEV * jax.random.uniform(every_key[2], (SEQUENCE_TOTAL, HEADS, 1), minval=0.06, maxval=0.2))
    decay_rates = jnp.where(slow_heads, slow_rate, fast_rate)
    block_multiplier = jnp.exp(jax.random.uniform(every_key[3], (SEQUENCE_TOTAL, HEADS, CACHE_POSITIONS // POS_DEV), minval=-0.7, maxval=0.7))
    block_multiplier = jnp.repeat(block_multiplier, POS_DEV, axis=2)
    coarse_estimate = jax.random.uniform(every_key[4], (SEQUENCE_TOTAL, HEADS, CACHE_POSITIONS), minval=0.3, maxval=1.7)
    flurry_position = jax.random.randint(every_key[5], (SEQUENCE_TOTAL, 1, 2), 0, CACHE_POSITIONS)
    position_numbers = jnp.arange(CACHE_POSITIONS, dtype=jnp.int32)[None, None, :]
    flurry_groups = ((position_numbers == flurry_position[..., 0:1]) | (position_numbers == flurry_position[..., 1:2])).astype(jnp.float32)
    tree_depth = jax.random.uniform(every_key[6], (SEQUENCE_TOTAL, HEADS, 1), minval=0.22, maxval=0.69)
    logarithm_gates = -decay_rates * block_multiplier * coarse_estimate - flurry_groups * tree_depth
    return jnp.cumsum(logarithm_gates, axis=2).astype(jnp.float32)


def draw_parents(key, part):
    draws = jax.random.randint(key, (SEQUENCE_TOTAL, PROPS), 0, 3, dtype=jnp.int32)
    step_ids = jnp.arange(PROPS, dtype=jnp.int32)[None, :]
    back_steps = draws % jnp.maximum(jnp.minimum(step_ids, 3), 1)
    return jnp.where(step_ids == 0, -1, step_ids - 1 - back_steps).astype(jnp.int32)


def with_ends(values, key, low, high):
    longest = values.shape.index(max(values.shape))
    spots = []
    for shift in (0, 1):
        where = [jax.random.randint(jax.random.fold_in(key, axis), (), 0, length) for axis, length in enumerate(values.shape)]
        where[longest] = (where[longest] + shift) % values.shape[longest]
        spots.append(tuple(where))
    return values.at[spots[0]].set(low).at[spots[1]].set(high)


def block_levels(rng, shape, cuts, low, top_value):
    level, own = 1.0, jax.random.fold_in(rng, 6)
    for axis_at, shards_of in cuts:
        heights = jnp.exp(jax.random.uniform(jax.random.fold_in(own, axis_at), (shards_of,), jnp.float32, low / len(cuts), top_value / len(cuts)))
        level = level * jnp.repeat(heights, shape[axis_at] // shards_of).reshape([-1 if axis == axis_at else 1 for axis in range(len(shape))])
    return level


def gaussian(key, dims, width, most, shards=(), kind=jnp.bfloat16):
    gain = block_levels(key, dims, shards, -0.22, 0.18) if shards else 1.0
    drawn = jax.random.normal(key, dims, jnp.float32) * width * gain
    return jnp.minimum(jnp.maximum(drawn, -most), most).astype(kind)


def setup_inputs(seed: int = 0) -> dict:
    arg_keys = jax.random.split(jax.random.key(seed), 18)
    tokens = gaussian(arg_keys[0], (SEQUENCE_TOTAL, PROPS, D), 1.0, 6.0, ((0, 4), (2, 4)))
    norm_gain = jnp.clip(1.0 + 0.18 * jax.random.normal(arg_keys[1], (D,), jnp.float32), 0.1, 1.9)
    w_query = gaussian(arg_keys[2], (D, HW), D ** -0.5, 0.125, ((0, 4), (1, 2)))
    w_key = gaussian(arg_keys[3], (D, HW), D ** -0.5, 0.125, ((0, 4), (1, 2)))
    w_value = gaussian(arg_keys[4], (D, HW), D ** -0.5, 0.125, ((0, 4), (1, 2)))
    w_forget = gaussian(arg_keys[5], (D, HEADS), D ** -0.5, 0.125)
    forget_bias = jnp.clip(jax.random.uniform(arg_keys[6], (HEADS,), jnp.float32, -2.0, 4.0), -2.0, 4.0)
    query_gain = jnp.clip(1.0 + 0.18 * jax.random.normal(arg_keys[7], (DH,), jnp.float32), 0.1, 1.9)
    key_gain = jnp.clip(1.0 + 0.18 * jax.random.normal(arg_keys[8], (DH,), jnp.float32), 0.1, 1.9)
    head_gain = jnp.clip(1.0 + 0.18 * jax.random.normal(arg_keys[9], (DH,), jnp.float32), 0.1, 1.9)
    w_out = gaussian(arg_keys[10], (HW, D), HW ** -0.5, 0.1875, ((0, 2), (1, 4)))
    key_cache = draw_key_cache(jax.random.fold_in(arg_keys[17], 71), 0)
    value_cache = gaussian(arg_keys[12], (SEQUENCE_TOTAL, CACHE_POSITIONS, HW), 1.0, 6.0, ((0, 4), (1, 4), (2, 2)))
    gate_cache = draw_gate_cache(jax.random.fold_in(arg_keys[17], 71), 0)
    lengths = with_ends(jax.random.randint(arg_keys[14], (SEQUENCE_TOTAL,), CACHE_POSITIONS - PROPS - ACCEPT_MOST + 1 - 2 * POS_DEV, CACHE_POSITIONS - PROPS - ACCEPT_MOST + 1), jax.random.fold_in(arg_keys[14], 1), CACHE_POSITIONS - PROPS - ACCEPT_MOST + 1 - 2 * POS_DEV, CACHE_POSITIONS - PROPS - ACCEPT_MOST).astype(jnp.int32)
    accepted = with_ends(jax.random.randint(arg_keys[15], (SEQUENCE_TOTAL,), 0, ACCEPT_MOST + 1), jax.random.fold_in(arg_keys[15], 1), 0, ACCEPT_MOST).astype(jnp.int32)
    parents = draw_parents(jax.random.fold_in(arg_keys[17], 71), 0)
    return dict(tokens=tokens, norm_gain=norm_gain, w_query=w_query, w_key=w_key, w_value=w_value, w_forget=w_forget, forget_bias=forget_bias, query_gain=query_gain, key_gain=key_gain, head_gain=head_gain, w_out=w_out, key_cache=key_cache, value_cache=value_cache, gate_cache=gate_cache, lengths=lengths, accepted=accepted, parents=parents)


EPSILON = 1e-06
MASKED = -1e+30

def head_norm(head_rows, gain_vec):
    mean_square = lax.optimization_barrier(jnp.mean(head_rows * head_rows, axis=-1, keepdims=True))
    return head_rows * lax.rsqrt(mean_square + EPSILON) * gain_vec

def ancestry(parents):
    count_all = parents.shape[0]
    step_ids = jnp.arange(count_all, dtype=jnp.int32)
    step_matrix = (parents[:, None] == step_ids[None, :]).astype(jnp.float32)
    identity = jnp.eye(count_all, dtype=jnp.float32)

    def extend(turn_index, ancestors):
        return identity + jnp.dot(step_matrix, ancestors, precision=lax.Precision.HIGHEST)
    return lax.fori_loop(0, count_all, extend, identity)

def softmax_block(scores, live_mask, block_values):
    row_max = lax.optimization_barrier(jnp.max(scores, axis=-1))
    weights = jnp.where(live_mask, jnp.exp(scores - row_max[..., None]), 0.0)
    row_total = lax.optimization_barrier(jnp.sum(weights, axis=-1))
    rounded = lax.optimization_barrier(weights.astype(jnp.bfloat16)).astype(jnp.float32)
    weighted = jnp.einsum('hpk,khd->phd', rounded, block_values.astype(jnp.float32))
    return (row_max.T, row_total.T, weighted)

def combine(earlier, later):
    earlier_max, earlier_total, earlier_sum = earlier
    later_max, later_total, later_sum = later
    row_max = jnp.maximum(earlier_max, later_max)
    earlier_scale = jnp.exp(earlier_max - row_max)
    later_scale = jnp.exp(later_max - row_max)
    return (row_max, earlier_total * earlier_scale + later_total * later_scale, earlier_sum * earlier_scale[..., None] + later_sum * later_scale[..., None])

def one_sequence(items, shared):
    tokens, key_cache, value_cache, gate_cache, length, accept, parents = items
    norm_gain, w_query, w_key, w_value, w_forget, forget_bias, query_gain, key_gain, head_gain, w_out = shared
    token_rows = tokens.astype(jnp.float32)
    inverse = lax.rsqrt(lax.optimization_barrier(jnp.mean(token_rows * token_rows, axis=1)) + EPSILON)[:, None]
    scaled = (token_rows * norm_gain).astype(jnp.bfloat16)
    query_raw = jnp.dot(scaled, w_query, preferred_element_type=jnp.float32) * inverse
    key_raw = jnp.dot(scaled, w_key, preferred_element_type=jnp.float32) * inverse
    value_raw = jnp.dot(scaled, w_value, preferred_element_type=jnp.float32) * inverse
    gate_raw = jnp.dot(scaled, w_forget, preferred_element_type=jnp.float32) * inverse
    queries = head_norm(query_raw.reshape(PROPS, HEADS, DH), query_gain).astype(jnp.bfloat16)
    keys_new = head_norm(key_raw.reshape(PROPS, HEADS, DH), key_gain).astype(jnp.bfloat16)
    values_new = value_raw.astype(jnp.bfloat16).reshape(PROPS, HEADS, DH)
    logarithm_gates = jax.nn.log_sigmoid(gate_raw + forget_bias)
    ancestors = ancestry(parents)
    path_sum = jnp.dot(ancestors, logarithm_gates, precision=lax.Precision.HIGHEST)
    base_pos = length + accept
    boundary = lax.dynamic_slice_in_dim(gate_cache, base_pos - 1, 1, 1)[:, 0]
    score_scale = DH ** (-0.5)
    score_shift = boundary[:, None, None] + path_sum.T[:, :, None]
    key_blocks = key_cache.reshape(N_KV, POS_DEV, HEADS, DH)
    value_blocks = value_cache.reshape(N_KV, POS_DEV, HEADS, DH)
    gate_blocks = gate_cache.reshape(HEADS, N_KV, POS_DEV).transpose(1, 0, 2)
    block_starts = jnp.arange(N_KV, dtype=jnp.int32) * POS_DEV
    query_wide = queries.astype(jnp.float32)

    def cache_block(block_args):
        block_keys, block_values, block_gates, block_start = block_args
        scores = jnp.einsum('phd,khd->hpk', query_wide, block_keys.astype(jnp.float32)) * score_scale
        scores = scores + score_shift - block_gates[:, None, :]
        live_mask = (block_start + jnp.arange(POS_DEV, dtype=jnp.int32) < base_pos)[None, None, :]
        scores = jnp.where(live_mask, scores, MASKED)
        return softmax_block(scores, live_mask, block_values)
    block_max, block_total, block_sum = lax.map(cache_block, (key_blocks, value_blocks, gate_blocks, block_starts))
    row_max = lax.optimization_barrier(jnp.max(block_max, axis=0))
    factors = jnp.exp(block_max - row_max)
    cache_part = (row_max, lax.optimization_barrier(jnp.sum(block_total * factors, axis=0)), lax.optimization_barrier(jnp.sum(block_sum * factors[..., None], axis=0)))
    tree_scores = jnp.einsum('phd,jhd->hpj', query_wide, keys_new.astype(jnp.float32)) * score_scale
    tree_scores = tree_scores + path_sum.T[:, :, None] - path_sum.T[:, None, :]
    tree_live = (ancestors > 0.5)[None]
    tree_scores = jnp.where(tree_live, tree_scores, MASKED)
    tree_part = softmax_block(tree_scores, tree_live, values_new)
    row_max, row_total, weighted = combine(cache_part, tree_part)
    attended = weighted / row_total[..., None]
    normed = head_norm(attended, head_gain).astype(jnp.bfloat16).reshape(PROPS, HW)
    group_width = HEAD_GROUP * DH
    layer_sum = jnp.zeros((PROPS, D), jnp.float32)
    for group_index in range(N_TP):
        lower = group_index * group_width
        group_term = jnp.dot(normed[:, lower:lower + group_width], w_out[lower:lower + group_width], preferred_element_type=jnp.float32)
        layer_sum = layer_sum + lax.optimization_barrier(group_term.astype(jnp.bfloat16)).astype(jnp.float32)
    layer_out = layer_sum.astype(jnp.bfloat16)
    zero_index = jnp.zeros((), jnp.int32)
    new_keys = lax.dynamic_update_slice(key_cache, keys_new.reshape(PROPS, HW), (base_pos, zero_index))
    new_values = lax.dynamic_update_slice(value_cache, values_new.reshape(PROPS, HW), (base_pos, zero_index))
    return (layer_out, new_keys, new_values, logarithm_gates)

def reference(tokens, norm_gain, w_query, w_key, w_value, w_forget, forget_bias, query_gain, key_gain, head_gain, w_out, key_cache, value_cache, gate_cache, lengths, accepted, parents):
    shared = (norm_gain, w_query, w_key, w_value, w_forget, forget_bias, query_gain, key_gain, head_gain, w_out)

    def per_sequence(items):
        return one_sequence(items, shared)
    layer_out, new_keys, new_values, proposal_gates = lax.map(per_sequence, (tokens, key_cache, value_cache, gate_cache, lengths, accepted, parents))
    return (layer_out, new_keys, new_values, proposal_gates)
```

```python
import functools

import jax
import jax.numpy as jnp
from jax import lax
from jax.experimental import pallas as pl
from jax.experimental.pallas import tpu as pltpu
from jax.sharding import PartitionSpec as P

EPSILON = 1e-06
MASKED = -1e30


def head_norm(head_rows, gain_vec):
    mean_square = jnp.mean(head_rows * head_rows, axis=-1, keepdims=True)
    return head_rows * lax.rsqrt(mean_square + EPSILON) * gain_vec


def ancestry(parents):
    count_all = parents.shape[1]
    step_ids = jnp.arange(count_all, dtype=jnp.int32)
    step_matrix = (parents[:, :, None] == step_ids[None, None, :]).astype(jnp.float32)
    identity = jnp.broadcast_to(jnp.eye(count_all, dtype=jnp.float32), step_matrix.shape)

    def extend(turn_index, ancestors):
        return identity + jnp.einsum(
            "sij,sjk->sik", step_matrix, ancestors, precision=lax.Precision.HIGHEST
        )

    return lax.fori_loop(0, count_all, extend, identity)


def combine(earlier, later):
    earlier_max, earlier_total, earlier_sum = earlier
    later_max, later_total, later_sum = later
    row_max = jnp.maximum(earlier_max, later_max)
    earlier_scale = jnp.exp(earlier_max - row_max)
    later_scale = jnp.exp(later_max - row_max)
    spread = earlier_max.shape + (-1,)
    joined = (
        earlier_sum.reshape(spread) * earlier_scale[..., None]
        + later_sum.reshape(spread) * later_scale[..., None]
    )
    return (
        row_max,
        earlier_total * earlier_scale + later_total * later_scale,
        joined.reshape(earlier_sum.shape),
    )


def block_part(scores, live_mask, block_values):
    seq_count, heads_local, prop_count, key_count = scores.shape
    row_max = jnp.max(scores, axis=3)
    weights = jnp.where(live_mask, jnp.exp(scores - row_max[..., None]), 0.0)
    row_total = jnp.sum(weights, axis=3)
    weighted = jnp.einsum(
        "shpk,skhd->sphd",
        weights.astype(jnp.bfloat16),
        block_values,
        preferred_element_type=jnp.float32,
    )
    return (
        jnp.transpose(row_max, (0, 2, 1)),
        jnp.transpose(row_total, (0, 2, 1)),
        weighted.reshape(seq_count, prop_count, -1),
    )


def finish_rows(row_sums, inverse, query_gain, key_gain, heads_local):
    head_width = row_sums.shape[1] // 3
    head_size = head_width // heads_local
    row_count = row_sums.shape[0]
    raw_sums = row_sums * inverse[:, None]
    queries = head_norm(
        raw_sums[:, :head_width].reshape(row_count, heads_local, head_size), query_gain
    )
    keyed = head_norm(
        raw_sums[:, head_width : 2 * head_width].reshape(row_count, heads_local, head_size),
        key_gain,
    )
    return jnp.concatenate(
        [
            queries.reshape(row_count, head_width),
            keyed.reshape(row_count, head_width),
            raw_sums[:, 2 * head_width :],
        ],
        axis=1,
    ).astype(jnp.bfloat16)


def flatten_part(part_triple, rows_all):
    part_max, part_total, part_sum = part_triple
    return (
        part_max.reshape(rows_all, -1),
        part_total.reshape(rows_all, -1),
        part_sum.reshape(rows_all, -1),
    )


def shards(
    tokens,
    norm_gain,
    w_query,
    w_key,
    w_value,
    w_forget,
    forget_bias,
    query_gain,
    key_gain,
    head_gain,
    w_out,
    key_cache,
    value_cache,
    gate_cache,
    lengths,
    accepted,
    parents,
):
    seq_count, prop_count, width_in = tokens.shape
    pos_dev = key_cache.shape[1]
    heads_local = gate_cache.shape[1]
    head_width = key_cache.shape[2]
    head_size = head_width // heads_local
    rows_all = seq_count * prop_count
    full_width = w_forget.shape[0]
    kv_index = lax.axis_index("kv")
    tp_index = lax.axis_index("tp")
    flattened = tokens.reshape(rows_all, width_in).astype(jnp.float32)
    squares = jnp.sum(flattened * flattened, axis=1)
    scaled = (flattened * norm_gain).astype(jnp.bfloat16)
    w_rows = lax.dynamic_slice_in_dim(w_forget, kv_index * width_in, width_in, 0)
    gate_part = jnp.dot(scaled, w_rows, preferred_element_type=jnp.float32)
    w_joined = jnp.concatenate([w_query, w_key, w_value], axis=1)
    summed, gate_sum, square_sum = lax.psum(
        (jnp.dot(scaled, w_joined, preferred_element_type=jnp.float32), gate_part, squares), "kv"
    )
    inverse = lax.rsqrt(square_sum / full_width + EPSILON)
    joined = finish_rows(summed, inverse, query_gain, key_gain, heads_local)
    log_all = jax.nn.log_sigmoid(gate_sum * inverse[:, None] + forget_bias)
    log_own = lax.dynamic_slice_in_dim(log_all, tp_index * heads_local, heads_local, 1)
    log_own = log_own.reshape(seq_count, prop_count, heads_local)
    queries = joined[:, :head_width].reshape(seq_count, prop_count, heads_local, head_size)
    keys_new = joined[:, head_width : 2 * head_width].reshape(
        seq_count, prop_count, heads_local, head_size
    )
    values_new = joined[:, 2 * head_width :].reshape(seq_count, prop_count, heads_local, head_size)
    ancestors = ancestry(parents)
    path_sum = jnp.einsum("sij,sjh->sih", ancestors, log_own, precision=lax.Precision.HIGHEST)
    base_pos = lengths + accepted
    positions = kv_index * pos_dev + jnp.arange(pos_dev, dtype=jnp.int32)
    score_scale = head_size ** (-0.5)
    cached_keys = key_cache.reshape(seq_count, pos_dev, heads_local, head_size)
    cached_values = value_cache.reshape(seq_count, pos_dev, heads_local, head_size)
    scores = jnp.einsum("sphd,skhd->shpk", queries, cached_keys, preferred_element_type=jnp.float32)
    scores = scores * score_scale - gate_cache[:, :, None, :]
    live_mask = (positions[None, :] < base_pos[:, None])[:, None, None, :]
    scores = jnp.where(live_mask, scores, MASKED)
    local_part = block_part(scores, live_mask, cached_values)
    hit_mask = positions[None, :] == (base_pos - 1)[:, None]
    boundary_local = jnp.sum(jnp.where(hit_mask[:, None, :], gate_cache, 0.0), axis=2)
    tree_live = (ancestors > 0.5)[:, None, :, :]
    boundary = lax.psum(boundary_local, "kv")
    flat_max, flat_total, flat_sum = flatten_part(local_part, rows_all)
    got_max, got_total, got_sum = (
        lax.all_to_all(flat_max[None], "kv", split_axis=1, concat_axis=0, tiled=True),
        lax.all_to_all(flat_total[None], "kv", split_axis=1, concat_axis=0, tiled=True),
        lax.all_to_all(flat_sum[None], "kv", split_axis=1, concat_axis=0, tiled=True),
    )
    top = jnp.max(got_max, axis=0)
    factors = jnp.exp(got_max - top[None])
    own_rows = got_max.shape[1]
    summed_rows = jnp.sum(
        got_sum.reshape(got_sum.shape[0], own_rows, heads_local, head_size) * factors[..., None],
        axis=0,
    )
    merged = (top, jnp.sum(got_total * factors, axis=0), summed_rows.reshape(own_rows, head_width))
    tree_scores = jnp.einsum(
        "sphd,sjhd->shpj", queries, keys_new, preferred_element_type=jnp.float32
    )
    tree_scores = (
        tree_scores * score_scale
        - jnp.transpose(path_sum, (0, 2, 1))[:, :, None, :]
        - boundary[:, :, None, None]
    )
    tree_scores = jnp.where(tree_live, tree_scores, MASKED)
    tree_max, tree_total, tree_sum = flatten_part(
        block_part(tree_scores, tree_live, values_new), rows_all
    )
    row_lower = kv_index * own_rows
    merged = combine(
        merged,
        (
            lax.dynamic_slice_in_dim(tree_max, row_lower, own_rows, 0),
            lax.dynamic_slice_in_dim(tree_total, row_lower, own_rows, 0),
            lax.dynamic_slice_in_dim(tree_sum, row_lower, own_rows, 0),
        ),
    )
    row_max, row_total, weighted = merged
    attended = weighted.reshape(own_rows, heads_local, head_size) / row_total[..., None]
    own_normed = head_norm(attended, head_gain).astype(jnp.bfloat16).reshape(own_rows, head_width)
    normed = lax.all_gather(own_normed, "kv", axis=0, tiled=True)
    out_term = jnp.dot(normed, w_out, preferred_element_type=jnp.float32)
    layer_out = lax.psum(out_term.astype(jnp.bfloat16), "tp")
    layer_out = layer_out.reshape(seq_count, prop_count, -1)
    new_rows = jnp.concatenate(
        [
            keys_new.reshape(seq_count, prop_count, head_width),
            values_new.reshape(seq_count, prop_count, head_width),
        ],
        axis=2,
    )
    slot_index = positions[None, :, None] - base_pos[:, None, None]
    placing = slot_index == jnp.arange(prop_count, dtype=jnp.int32)[None, None, :]
    written = jnp.einsum(
        "skp,spc->skc", placing.astype(jnp.bfloat16), new_rows, preferred_element_type=jnp.float32
    ).astype(jnp.bfloat16)
    hit_rows = jnp.any(placing, axis=2)[..., None]
    new_keys = jnp.where(hit_rows, written[..., :head_width], key_cache)
    new_values = jnp.where(hit_rows, written[..., head_width:], value_cache)
    return (layer_out, new_keys, new_values, log_own)


MESH = pl.DeviceIdType.MESH
LANES = 128


def tile_head_norm(rows, gain_row, head_size):
    lane = lax.broadcasted_iota(jnp.int32, (rows.shape[0], LANES), 1)
    low = lane < head_size
    parts = []
    for start in range(0, rows.shape[1], LANES):
        part = rows[:, start : start + LANES]
        square = part * part
        first = jnp.sum(jnp.where(low, square, 0.0), axis=1, keepdims=True) / head_size
        second = jnp.sum(jnp.where(low, 0.0, square), axis=1, keepdims=True) / head_size
        parts.append(part * lax.rsqrt(jnp.where(low, first, second) + EPSILON) * gain_row)
    return jnp.concatenate(parts, axis=1)


def spread_heads(stats, offset, heads, head_size):
    lane = lax.broadcasted_iota(jnp.int32, (stats.shape[0], LANES), 1)
    return jnp.concatenate(
        [
            jnp.where(
                lane < head_size,
                stats[:, offset + head : offset + head + 1],
                stats[:, offset + head + 1 : offset + head + 2],
            )
            for head in range(0, heads, 2)
        ],
        axis=1,
    )


def attend_rows(queries, keys, values, adjust, live, heads, head_size, scale):
    props = queries.shape[0]
    quad = 4
    width = quad * head_size
    row_head = lax.broadcasted_iota(jnp.int32, (quad * props, width), 0) // props
    col_head = lax.broadcasted_iota(jnp.int32, (quad * props, width), 1) // head_size
    own = (row_head == col_head).astype(jnp.float32).astype(jnp.bfloat16)
    lane = lax.broadcasted_iota(jnp.int32, (props, LANES), 1)
    tiles, peaks, totals = [], [], []
    for group in range(heads // quad):
        columns = slice(group * width, (group + 1) * width)
        stacked = jnp.concatenate([queries[:, columns]] * quad, axis=0) * own
        scores = lax.dot_general(
            stacked, keys[:, columns], (((1,), (1,)), ((), ())), preferred_element_type=jnp.float32
        )
        weights = []
        for inner in range(quad):
            head = group * quad + inner
            part = scores[inner * props : (inner + 1) * props] * scale - adjust(head)
            part = jnp.where(live, part, MASKED)
            peak = jnp.max(part, axis=1, keepdims=True)
            weight = jnp.where(live, jnp.exp(part - peak), 0.0)
            peaks.append(peak)
            totals.append(jnp.sum(weight, axis=1, keepdims=True))
            weights.append(weight.astype(jnp.bfloat16))
        summed = jnp.dot(
            jnp.concatenate(weights, axis=0), values[:, columns], preferred_element_type=jnp.float32
        )
        for pair in range(quad // 2):
            cols = slice(pair * LANES, (pair + 1) * LANES)
            first = summed[2 * pair * props : (2 * pair + 1) * props, cols]
            second = summed[(2 * pair + 1) * props : (2 * pair + 2) * props, cols]
            tiles.append(jnp.where(lane < head_size, first, second))
    return jnp.concatenate(tiles, axis=1), peaks, totals


def pack_stats(columns, props):
    lane = lax.broadcasted_iota(jnp.int32, (props, LANES), 1)
    stats = jnp.zeros((props, LANES), jnp.float32)
    for index, column in enumerate(columns):
        stats = jnp.where(lane == index, column, stats)
    return stats


def layer_kernel(
    sizes,
    lengths,
    accepted,
    parents,
    tokens,
    norm_gain,
    w_query,
    w_key,
    w_value,
    w_forget,
    forget_bias,
    query_gain,
    key_gain,
    head_gain,
    w_out,
    key_cache,
    value_cache,
    gate_cache,
    out_layer,
    out_rows,
    out_gates,
    tok_v,
    norm_v,
    wq_v,
    wk_v,
    wv_v,
    wf_v,
    bias_v,
    qgain_v,
    kgain_v,
    hgain_v,
    wo_v,
    kc_v,
    vc_v,
    gc_v,
    send_q,
    send_kv,
    got_q,
    got_kv,
    all_q,
    all_gates,
    all_kv,
    send_part,
    got_part,
    all_normed,
    term_own,
    term_other,
    load_sem,
    sent_sem,
    came_sem,
    pair_sem,
):
    n, heads, head_size, full_width = sizes
    me = lax.axis_index("kv")
    core = lax.axis_index("tp")
    seqs, props, width_in = tok_v.shape
    head_width = heads * head_size
    pos_dev = kc_v.shape[1]
    rows_all = seqs * props
    scale = head_size ** (-0.5)
    order = sorted(range(1, n), key=lambda step: abs(2 * step - n))

    forget_rows = pl.ds(pl.multiple_of(me * width_in, width_in), width_in)
    loads = {}
    for index, (name, source, target) in enumerate(
        (
            ("tokens", tokens, tok_v),
            ("norm", norm_gain, norm_v),
            ("wq", w_query, wq_v),
            ("wf", w_forget.at[forget_rows], wf_v),
            ("bias", forget_bias, bias_v),
            ("qgain", query_gain, qgain_v),
            ("kgain", key_gain, kgain_v),
            ("hgain", head_gain, hgain_v),
            ("wk", w_key, wk_v),
            ("wv", w_value, wv_v),
            ("gates", gate_cache, gc_v),
            ("keys", key_cache, kc_v),
            ("values", value_cache, vc_v),
            ("wo", w_out, wo_v),
        )
    ):
        loads[name] = pltpu.make_async_copy(source, target, load_sem.at[index])
        loads[name].start()

    barrier = pltpu.get_barrier_semaphore()
    for step in order:
        pl.semaphore_signal(
            barrier, inc=1, device_id={"kv": lax.rem(me + step, n)}, device_id_type=MESH
        )
    pl.semaphore_signal(barrier, inc=1, device_id={"tp": 1 - core}, device_id_type=MESH)

    sent = []

    def push(phase, step, source, target):
        peer = lax.rem(me + step, n)
        copy = pltpu.make_async_remote_copy(
            src_ref=source(peer),
            dst_ref=target.at[me],
            send_sem=sent_sem.at[phase, step],
            recv_sem=came_sem.at[phase, me],
            device_id={"kv": peer},
            device_id_type=MESH,
        )
        copy.start()
        sent.append(copy)

    def arrive(phase, step, target):
        peer = lax.rem(me + step, n)
        pltpu.make_async_remote_copy(
            src_ref=target.at[peer],
            dst_ref=target.at[peer],
            send_sem=sent_sem.at[phase, step],
            recv_sem=came_sem.at[phase, peer],
            device_id={"kv": peer},
            device_id_type=MESH,
        ).wait_recv()

    loads["tokens"].wait()
    loads["norm"].wait()
    flat = tok_v[...].astype(jnp.float32).reshape(rows_all, width_in)
    squares = jnp.sum(flat * flat, axis=1, keepdims=True)
    scaled = (flat * norm_v[...]).astype(jnp.bfloat16)
    loads["wq"].wait()
    loads["wf"].wait()
    send_q[:, :, :head_width] = jnp.dot(
        scaled, wq_v[...], preferred_element_type=jnp.float32
    ).reshape(seqs, props, head_width)
    gate_part = jnp.dot(scaled, wf_v[...], preferred_element_type=jnp.float32)
    gate_heads = gate_part.shape[1]
    send_q[:, :, head_width:] = jnp.broadcast_to(squares, (rows_all, LANES)).reshape(
        seqs, props, LANES
    )
    send_q[:, :, head_width : head_width + gate_heads] = gate_part.reshape(seqs, props, gate_heads)
    pl.semaphore_wait(barrier, n)
    for step in order:
        push(0, step, lambda peer: send_q.at[peer], got_q)

    loads["wk"].wait()
    send_kv[:, :, :head_width] = jnp.dot(
        scaled, wk_v[...], preferred_element_type=jnp.float32
    ).reshape(seqs, props, head_width)
    loads["wv"].wait()
    send_kv[:, :, head_width:] = jnp.dot(
        scaled, wv_v[...], preferred_element_type=jnp.float32
    ).reshape(seqs, props, head_width)

    row = lax.broadcasted_iota(jnp.int32, (LANES, LANES), 0)
    column = lax.broadcasted_iota(jnp.int32, (LANES, LANES), 1)
    eye = (row == column).astype(jnp.float32)
    target_column = jnp.full((LANES, LANES), -1, jnp.int32)
    for prop in range(props):
        target_column = jnp.where(row == prop, parents[me, prop], target_column)
    power = (target_column == column).astype(jnp.float32)
    ancestors = eye + power
    reach = 2
    while reach < props:
        half = power.astype(jnp.bfloat16)
        power = jnp.dot(half, half, preferred_element_type=jnp.float32)
        ancestors = ancestors + jnp.dot(
            ancestors.astype(jnp.bfloat16),
            power.astype(jnp.bfloat16),
            preferred_element_type=jnp.float32,
        )
        reach *= 2
    for name in ("bias", "qgain", "kgain", "hgain"):
        loads[name].wait()
    gain_q = jnp.concatenate([qgain_v[...]] * (LANES // head_size), axis=1)
    gain_k = jnp.concatenate([kgain_v[...]] * (LANES // head_size), axis=1)
    gain_h = jnp.concatenate([hgain_v[...]] * (LANES // head_size), axis=1)

    for step in order:
        arrive(0, step, got_q)
    raw = send_q[me]
    for step in range(1, n):
        raw = raw + got_q[lax.rem(me + step, n)]
    small = raw[:, head_width:]
    inverse = lax.rsqrt(small[:, gate_heads : gate_heads + 1] / full_width + EPSILON)
    all_q[me] = tile_head_norm(raw[:, :head_width] * inverse, gain_q, head_size).astype(
        jnp.bfloat16
    )
    for step in order:
        push(1, step, lambda peer: all_q.at[me], all_q)
    logits = small[:, :gate_heads] * inverse + bias_v[...]
    logs = -(jnp.maximum(-logits, 0.0) + jnp.log1p(jnp.exp(-jnp.abs(logits))))
    logs = jnp.where(core == 0, logs[:, :heads], logs[:, heads:])
    all_gates[me] = jnp.zeros((props, LANES), jnp.float32)
    all_gates[me, :, :heads] = logs
    for step in order:
        push(2, step, lambda peer: send_kv.at[peer], got_kv)
    for step in order:
        push(3, step, lambda peer: all_gates.at[me], all_gates)

    lane_pos = me * pos_dev + lax.broadcasted_iota(jnp.int32, (props, pos_dev), 1)
    loads["gates"].wait()
    loads["keys"].wait()
    loads["values"].wait()
    for step in [0] + order:
        seq = lax.rem(me + step, n)
        if step:
            arrive(1, step, all_q)
        base = lengths[seq] + accepted[seq]
        gate_rows = gc_v[seq]
        hit = lane_pos == base - 1
        total, peaks, totals = attend_rows(
            all_q[seq],
            kc_v[seq],
            vc_v[seq],
            lambda head: gate_rows[head : head + 1],
            lane_pos < base,
            heads,
            head_size,
            scale,
        )
        edges = [
            jnp.sum(
                jnp.where(hit[:1], gate_rows[head : head + 1], 0.0), axis=1, keepdims=True
            )
            for head in range(heads)
        ]
        send_part[seq, :, :head_width] = total
        send_part[seq, :, head_width:] = pack_stats(peaks + totals + edges, props)
        if step:
            push(4, step, lambda peer: send_part.at[peer], got_part)

    for step in order:
        arrive(2, step, got_kv)
    raw = send_kv[me]
    for step in range(1, n):
        raw = raw + got_kv[lax.rem(me + step, n)]
    raw = raw * inverse
    keys_own = tile_head_norm(raw[:, :head_width], gain_k, head_size).astype(jnp.bfloat16)
    values_own = raw[:, head_width:].astype(jnp.bfloat16)
    all_kv[me, :, :head_width] = keys_own
    all_kv[me, :, head_width:] = values_own
    for step in order:
        push(5, step, lambda peer: all_kv.at[me], all_kv)

    padding = jnp.zeros((LANES - props, head_width), jnp.bfloat16)
    log_tile = jnp.concatenate(
        [all_gates[me], jnp.zeros((LANES - props, LANES), jnp.float32)], axis=0
    )
    path_sum = jnp.dot(ancestors, log_tile, precision=lax.Precision.HIGHEST)
    on_diagonal = row == column
    tree_sum, tree_peaks, tree_totals = attend_rows(
        all_q[me],
        jnp.concatenate([keys_own, padding], axis=0),
        jnp.concatenate([values_own, padding], axis=0),
        lambda head: jnp.sum(
            jnp.where(on_diagonal, path_sum[:, head : head + 1], 0.0), axis=0, keepdims=True
        ),
        ancestors[:props] > 0.5,
        heads,
        head_size,
        scale,
    )
    tree_stats = pack_stats(tree_peaks + tree_totals, props)

    for step in order:
        arrive(4, step, got_part)
    parts = [send_part[me]] + [got_part[lax.rem(me + step, n)] for step in range(1, n)]
    edge = functools.reduce(jnp.add, [part[:, head_width:] for part in parts])
    tops = [spread_heads(part[:, head_width:], 0, heads, head_size) for part in parts]
    sums = [spread_heads(part[:, head_width:], heads, heads, head_size) for part in parts]
    numbers = [part[:, :head_width] for part in parts]
    tops.append(
        spread_heads(tree_stats, 0, heads, head_size)
        - spread_heads(edge, 2 * heads, heads, head_size)
    )
    sums.append(spread_heads(tree_stats, heads, heads, head_size))
    numbers.append(tree_sum)
    top = functools.reduce(jnp.maximum, tops)
    factors = [jnp.exp(each - top) for each in tops]
    weighted = functools.reduce(jnp.add, [x * y for x, y in zip(numbers, factors)])
    row_total = functools.reduce(jnp.add, [x * y for x, y in zip(sums, factors)])
    all_normed[me] = tile_head_norm(weighted / row_total, gain_h, head_size).astype(jnp.bfloat16)
    for step in order:
        push(6, step, lambda peer: all_normed.at[me], all_normed)
    loads["wo"].wait()
    for step in order:
        arrive(6, step, all_normed)
    term_own[...] = jnp.dot(
        all_normed[...].reshape(rows_all, head_width),
        wo_v[...],
        preferred_element_type=jnp.float32,
    ).astype(jnp.bfloat16)
    pair = pltpu.make_async_remote_copy(
        src_ref=term_own,
        dst_ref=term_other,
        send_sem=pair_sem.at[0],
        recv_sem=pair_sem.at[1],
        device_id={"tp": 1 - core},
        device_id_type=MESH,
    )
    pair.start()
    for step in order:
        arrive(3, step, all_gates)
    for step in order:
        arrive(5, step, all_kv)
    out_gates[...] = all_gates[:, :, :heads]
    out_rows[...] = all_kv[...]
    pair.wait()
    joined = term_own[...].astype(jnp.float32) + term_other[...].astype(jnp.float32)
    out_layer[...] = joined.astype(jnp.bfloat16).reshape(out_layer.shape)
    for copy in sent:
        copy.wait_send()


def write_kernel(
    lengths,
    accepted,
    layer_in,
    rows_in,
    gates_in,
    key_cache,
    value_cache,
    layer_out,
    new_keys,
    new_values,
    gates_out,
    kc_v,
    vc_v,
    in_sem,
    out_sem,
):
    seqs, pos_dev, head_width = kc_v.shape
    props = rows_in.shape[1]
    window = 2 * props
    start = lax.axis_index("kv") * pos_dev
    caches = ((key_cache, kc_v, new_keys), (value_cache, vc_v, new_values))
    loads = [
        [
            pltpu.make_async_copy(source.at[seq], held.at[seq], in_sem.at[side, seq])
            for side, (source, held, _) in enumerate(caches)
        ]
        for seq in range(seqs)
    ]
    for pair in loads:
        for copy in pair:
            copy.start()
    layer_out[...] = layer_in[...]
    gates_out[...] = gates_in[...]
    slot = lax.broadcasted_iota(jnp.int32, (window, props), 0)
    prop = lax.broadcasted_iota(jnp.int32, (window, props), 1)
    line = lax.broadcasted_iota(jnp.int32, (window, head_width), 0)
    stores = []
    for seq in range(seqs):
        offset = lengths[seq] + accepted[seq] - start
        inside = jnp.clip(offset, 0, pos_dev - 1)
        lower = jnp.minimum(inside // props * props, pos_dev - window)
        rows = pl.ds(pl.multiple_of(lower, props), window)
        placing = (slot + lower - offset == prop).astype(jnp.float32).astype(jnp.bfloat16)
        place = line + lower - offset
        hit = (place >= 0) & (place < props)
        for side, (_, held, target) in enumerate(caches):
            fresh = jnp.dot(
                placing,
                rows_in[seq, :, side * head_width : (side + 1) * head_width],
                preferred_element_type=jnp.float32,
            )
            loads[seq][side].wait()
            kept = held[seq, rows, :].astype(jnp.float32)
            held[seq, rows, :] = jnp.where(hit, fresh, kept).astype(jnp.bfloat16)
            copy = pltpu.make_async_copy(held.at[seq], target.at[seq], out_sem.at[side, seq])
            copy.start()
            stores.append(copy)
    for copy in stores:
        copy.wait()


def fused_shards(
    tokens,
    norm_gain,
    w_query,
    w_key,
    w_value,
    w_forget,
    forget_bias,
    query_gain,
    key_gain,
    head_gain,
    w_out,
    key_cache,
    value_cache,
    gate_cache,
    lengths,
    accepted,
    parents,
    n,
):
    seqs, props, width_in = tokens.shape
    pos_dev, head_width = key_cache.shape[1:]
    heads = gate_cache.shape[1]
    head_size = head_width // heads
    width_out = w_out.shape[1]
    bf16, f32 = jnp.bfloat16, jnp.float32
    smem = pl.BlockSpec(memory_space=pltpu.SMEM)
    vmem = pl.BlockSpec(memory_space=pltpu.VMEM)
    any_space = pl.BlockSpec(memory_space=pl.ANY)
    line = lambda vector: vector.reshape(1, -1)
    operands = (
        tokens,
        line(norm_gain),
        w_query,
        w_key,
        w_value,
        w_forget,
        line(forget_bias),
        line(query_gain),
        line(key_gain),
        line(head_gain),
        w_out,
        key_cache,
        value_cache,
        gate_cache,
    )
    part_width = head_width + LANES
    scratch = [
        pltpu.VMEM(tokens.shape, bf16),
        pltpu.VMEM((1, width_in), f32),
        pltpu.VMEM(w_query.shape, bf16),
        pltpu.VMEM(w_key.shape, bf16),
        pltpu.VMEM(w_value.shape, bf16),
        pltpu.VMEM((width_in, w_forget.shape[1]), bf16),
        pltpu.VMEM((1, forget_bias.shape[0]), f32),
        pltpu.VMEM((1, head_size), f32),
        pltpu.VMEM((1, head_size), f32),
        pltpu.VMEM((1, head_size), f32),
        pltpu.VMEM(w_out.shape, bf16),
        pltpu.VMEM(key_cache.shape, bf16),
        pltpu.VMEM(value_cache.shape, bf16),
        pltpu.VMEM(gate_cache.shape, f32),
        pltpu.VMEM((seqs, props, part_width), f32),
        pltpu.VMEM((seqs, props, 2 * head_width), f32),
        pltpu.VMEM((n, props, part_width), f32),
        pltpu.VMEM((n, props, 2 * head_width), f32),
        pltpu.VMEM((n, props, head_width), bf16),
        pltpu.VMEM((n, props, LANES), f32),
        pltpu.VMEM((n, props, 2 * head_width), bf16),
        pltpu.VMEM((seqs, props, part_width), f32),
        pltpu.VMEM((n, props, part_width), f32),
        pltpu.VMEM((n, props, head_width), bf16),
        pltpu.VMEM((seqs * props, width_out), bf16),
        pltpu.VMEM((seqs * props, width_out), bf16),
        pltpu.SemaphoreType.DMA((14,)),
        pltpu.SemaphoreType.DMA((7, n)),
        pltpu.SemaphoreType.DMA((7, n)),
        pltpu.SemaphoreType.DMA((2,)),
    ]
    layer, rows, gates = pl.pallas_call(
        functools.partial(layer_kernel, (n, heads, head_size, w_forget.shape[0])),
        out_shape=(
            jax.ShapeDtypeStruct((seqs, props, width_out), bf16),
            jax.ShapeDtypeStruct((seqs, props, 2 * head_width), bf16),
            jax.ShapeDtypeStruct((seqs, props, heads), f32),
        ),
        in_specs=[smem] * 3 + [any_space] * len(operands),
        out_specs=(vmem, vmem, vmem),
        scratch_shapes=scratch,
        compiler_params=pltpu.CompilerParams(collective_id=0, has_side_effects=True),
        name="layer",
    )(lengths, accepted, parents, *operands)
    return pl.pallas_call(
        write_kernel,
        out_shape=(
            jax.ShapeDtypeStruct(layer.shape, bf16),
            jax.ShapeDtypeStruct(key_cache.shape, bf16),
            jax.ShapeDtypeStruct(value_cache.shape, bf16),
            jax.ShapeDtypeStruct(gates.shape, f32),
        ),
        in_specs=[smem, smem, vmem, vmem, vmem, any_space, any_space],
        out_specs=(vmem, any_space, any_space, vmem),
        scratch_shapes=[
            pltpu.VMEM(key_cache.shape, bf16),
            pltpu.VMEM(value_cache.shape, bf16),
            pltpu.SemaphoreType.DMA((2, seqs)),
            pltpu.SemaphoreType.DMA((2, seqs)),
        ],
        name="write",
    )(lengths, accepted, layer, rows, gates, key_cache, value_cache)


def pick_shards(n, cores):
    def chosen(*arrays):
        tokens, key_cache, gate_cache = arrays[0], arrays[11], arrays[13]
        heads = gate_cache.shape[1]
        fits = (
            tokens.shape[0] == n
            and n > 1
            and cores == 2
            and tokens.shape[1] == 16
            and tokens.shape[2] % LANES == 0
            and key_cache.shape[2] == 64 * heads
            and heads % 4 == 0
            and 3 * heads <= LANES
        )
        return fused_shards(*arrays, n) if fits else shards(*arrays)

    return chosen


def solution(mesh):
    placed = (
        P("dp", None, "kv"),
        P("kv"),
        P("kv", "tp"),
        P("kv", "tp"),
        P("kv", "tp"),
        P(),
        P(),
        P(),
        P(),
        P(),
        P("tp", "kv"),
        P("dp", "kv", "tp"),
        P("dp", "kv", "tp"),
        P("dp", "tp", "kv"),
        P("dp"),
        P("dp"),
        P("dp", None),
    )
    return jax.shard_map(
        pick_shards(mesh.shape["kv"], mesh.shape["tp"]),
        mesh=mesh,
        in_specs=placed,
        out_specs=(
            P("dp", None, "kv"),
            P("dp", "kv", "tp"),
            P("dp", "kv", "tp"),
            P("dp", None, "tp"),
        ),
        check_vma=False,
    )
```

```python
import functools

import jax
import jax.numpy as jnp
from jax import lax
from jax.experimental import pallas as pl
from jax.experimental.pallas import tpu as pltpu
from jax.sharding import PartitionSpec as P

EPSILON = 1e-06
MASKED = -1e30


def head_norm(head_rows, gain_vec):
    mean_square = jnp.mean(head_rows * head_rows, axis=-1, keepdims=True)
    return head_rows * lax.rsqrt(mean_square + EPSILON) * gain_vec


def ancestry(parents):
    count_all = parents.shape[1]
    step_ids = jnp.arange(count_all, dtype=jnp.int32)
    step_matrix = (parents[:, :, None] == step_ids[None, None, :]).astype(jnp.float32)
    identity = jnp.broadcast_to(jnp.eye(count_all, dtype=jnp.float32), step_matrix.shape)

    def extend(turn_index, ancestors):
        return identity + jnp.einsum(
            "sij,sjk->sik", step_matrix, ancestors, precision=lax.Precision.HIGHEST
        )

    return lax.fori_loop(0, count_all, extend, identity)


def combine(earlier, later):
    earlier_max, earlier_total, earlier_sum = earlier
    later_max, later_total, later_sum = later
    row_max = jnp.maximum(earlier_max, later_max)
    earlier_scale = jnp.exp(earlier_max - row_max)
    later_scale = jnp.exp(later_max - row_max)
    spread = earlier_max.shape + (-1,)
    joined = (
        earlier_sum.reshape(spread) * earlier_scale[..., None]
        + later_sum.reshape(spread) * later_scale[..., None]
    )
    return (
        row_max,
        earlier_total * earlier_scale + later_total * later_scale,
        joined.reshape(earlier_sum.shape),
    )


def block_part(scores, live_mask, block_values):
    seq_count, heads_local, prop_count, key_count = scores.shape
    row_max = jnp.max(scores, axis=3)
    weights = jnp.where(live_mask, jnp.exp(scores - row_max[..., None]), 0.0)
    row_total = jnp.sum(weights, axis=3)
    weighted = jnp.einsum(
        "shpk,skhd->sphd",
        weights.astype(jnp.bfloat16),
        block_values,
        preferred_element_type=jnp.float32,
    )
    return (
        jnp.transpose(row_max, (0, 2, 1)),
        jnp.transpose(row_total, (0, 2, 1)),
        weighted.reshape(seq_count, prop_count, -1),
    )


def finish_rows(row_sums, inverse, query_gain, key_gain, heads_local):
    head_width = row_sums.shape[1] // 3
    head_size = head_width // heads_local
    row_count = row_sums.shape[0]
    raw_sums = row_sums * inverse[:, None]
    queries = head_norm(
        raw_sums[:, :head_width].reshape(row_count, heads_local, head_size), query_gain
    )
    keyed = head_norm(
        raw_sums[:, head_width : 2 * head_width].reshape(row_count, heads_local, head_size),
        key_gain,
    )
    return jnp.concatenate(
        [
            queries.reshape(row_count, head_width),
            keyed.reshape(row_count, head_width),
            raw_sums[:, 2 * head_width :],
        ],
        axis=1,
    ).astype(jnp.bfloat16)


def flatten_part(part_triple, rows_all):
    part_max, part_total, part_sum = part_triple
    return (
        part_max.reshape(rows_all, -1),
        part_total.reshape(rows_all, -1),
        part_sum.reshape(rows_all, -1),
    )


def shards(
    tokens,
    norm_gain,
    w_query,
    w_key,
    w_value,
    w_forget,
    forget_bias,
    query_gain,
    key_gain,
    head_gain,
    w_out,
    key_cache,
    value_cache,
    gate_cache,
    lengths,
    accepted,
    parents,
):
    seq_count, prop_count, width_in = tokens.shape
    pos_dev = key_cache.shape[1]
    heads_local = gate_cache.shape[1]
    head_width = key_cache.shape[2]
    head_size = head_width // heads_local
    rows_all = seq_count * prop_count
    full_width = w_forget.shape[0]
    kv_index = lax.axis_index("kv")
    tp_index = lax.axis_index("tp")
    flattened = tokens.reshape(rows_all, width_in).astype(jnp.float32)
    squares = jnp.sum(flattened * flattened, axis=1)
    scaled = (flattened * norm_gain).astype(jnp.bfloat16)
    w_rows = lax.dynamic_slice_in_dim(w_forget, kv_index * width_in, width_in, 0)
    gate_part = jnp.dot(scaled, w_rows, preferred_element_type=jnp.float32)
    w_joined = jnp.concatenate([w_query, w_key, w_value], axis=1)
    summed, gate_sum, square_sum = lax.psum(
        (jnp.dot(scaled, w_joined, preferred_element_type=jnp.float32), gate_part, squares), "kv"
    )
    inverse = lax.rsqrt(square_sum / full_width + EPSILON)
    joined = finish_rows(summed, inverse, query_gain, key_gain, heads_local)
    log_all = jax.nn.log_sigmoid(gate_sum * inverse[:, None] + forget_bias)
    log_own = lax.dynamic_slice_in_dim(log_all, tp_index * heads_local, heads_local, 1)
    log_own = log_own.reshape(seq_count, prop_count, heads_local)
    queries = joined[:, :head_width].reshape(seq_count, prop_count, heads_local, head_size)
    keys_new = joined[:, head_width : 2 * head_width].reshape(
        seq_count, prop_count, heads_local, head_size
    )
    values_new = joined[:, 2 * head_width :].reshape(seq_count, prop_count, heads_local, head_size)
    ancestors = ancestry(parents)
    path_sum = jnp.einsum("sij,sjh->sih", ancestors, log_own, precision=lax.Precision.HIGHEST)
    base_pos = lengths + accepted
    positions = kv_index * pos_dev + jnp.arange(pos_dev, dtype=jnp.int32)
    score_scale = head_size ** (-0.5)
    cached_keys = key_cache.reshape(seq_count, pos_dev, heads_local, head_size)
    cached_values = value_cache.reshape(seq_count, pos_dev, heads_local, head_size)
    scores = jnp.einsum("sphd,skhd->shpk", queries, cached_keys, preferred_element_type=jnp.float32)
    scores = scores * score_scale - gate_cache[:, :, None, :]
    live_mask = (positions[None, :] < base_pos[:, None])[:, None, None, :]
    scores = jnp.where(live_mask, scores, MASKED)
    local_part = block_part(scores, live_mask, cached_values)
    hit_mask = positions[None, :] == (base_pos - 1)[:, None]
    boundary_local = jnp.sum(jnp.where(hit_mask[:, None, :], gate_cache, 0.0), axis=2)
    tree_live = (ancestors > 0.5)[:, None, :, :]
    boundary = lax.psum(boundary_local, "kv")
    flat_max, flat_total, flat_sum = flatten_part(local_part, rows_all)
    got_max, got_total, got_sum = (
        lax.all_to_all(flat_max[None], "kv", split_axis=1, concat_axis=0, tiled=True),
        lax.all_to_all(flat_total[None], "kv", split_axis=1, concat_axis=0, tiled=True),
        lax.all_to_all(flat_sum[None], "kv", split_axis=1, concat_axis=0, tiled=True),
    )
    top = jnp.max(got_max, axis=0)
    factors = jnp.exp(got_max - top[None])
    own_rows = got_max.shape[1]
    summed_rows = jnp.sum(
        got_sum.reshape(got_sum.shape[0], own_rows, heads_local, head_size) * factors[..., None],
        axis=0,
    )
    merged = (top, jnp.sum(got_total * factors, axis=0), summed_rows.reshape(own_rows, head_width))
    tree_scores = jnp.einsum(
        "sphd,sjhd->shpj", queries, keys_new, preferred_element_type=jnp.float32
    )
    tree_scores = (
        tree_scores * score_scale
        - jnp.transpose(path_sum, (0, 2, 1))[:, :, None, :]
        - boundary[:, :, None, None]
    )
    tree_scores = jnp.where(tree_live, tree_scores, MASKED)
    tree_max, tree_total, tree_sum = flatten_part(
        block_part(tree_scores, tree_live, values_new), rows_all
    )
    row_lower = kv_index * own_rows
    merged = combine(
        merged,
        (
            lax.dynamic_slice_in_dim(tree_max, row_lower, own_rows, 0),
            lax.dynamic_slice_in_dim(tree_total, row_lower, own_rows, 0),
            lax.dynamic_slice_in_dim(tree_sum, row_lower, own_rows, 0),
        ),
    )
    row_max, row_total, weighted = merged
    attended = weighted.reshape(own_rows, heads_local, head_size) / row_total[..., None]
    own_normed = head_norm(attended, head_gain).astype(jnp.bfloat16).reshape(own_rows, head_width)
    normed = lax.all_gather(own_normed, "kv", axis=0, tiled=True)
    out_term = jnp.dot(normed, w_out, preferred_element_type=jnp.float32)
    layer_out = lax.psum(out_term.astype(jnp.bfloat16), "tp")
    layer_out = layer_out.reshape(seq_count, prop_count, -1)
    new_rows = jnp.concatenate(
        [
            keys_new.reshape(seq_count, prop_count, head_width),
            values_new.reshape(seq_count, prop_count, head_width),
        ],
        axis=2,
    )
    slot_index = positions[None, :, None] - base_pos[:, None, None]
    placing = slot_index == jnp.arange(prop_count, dtype=jnp.int32)[None, None, :]
    written = jnp.einsum(
        "skp,spc->skc", placing.astype(jnp.bfloat16), new_rows, preferred_element_type=jnp.float32
    ).astype(jnp.bfloat16)
    hit_rows = jnp.any(placing, axis=2)[..., None]
    new_keys = jnp.where(hit_rows, written[..., :head_width], key_cache)
    new_values = jnp.where(hit_rows, written[..., head_width:], value_cache)
    return (layer_out, new_keys, new_values, log_own)


MESH = pl.DeviceIdType.MESH
LANES = 128


def tile_head_norm(rows, gain_row, head_size):
    lane = lax.broadcasted_iota(jnp.int32, (rows.shape[0], LANES), 1)
    low = lane < head_size
    parts = []
    for start in range(0, rows.shape[1], LANES):
        part = rows[:, start : start + LANES]
        square = part * part
        first = jnp.sum(jnp.where(low, square, 0.0), axis=1, keepdims=True) / head_size
        second = jnp.sum(jnp.where(low, 0.0, square), axis=1, keepdims=True) / head_size
        parts.append(part * lax.rsqrt(jnp.where(low, first, second) + EPSILON) * gain_row)
    return jnp.concatenate(parts, axis=1)


def spread_heads(stats, offset, heads, head_size):
    lane = lax.broadcasted_iota(jnp.int32, (stats.shape[0], LANES), 1)
    return jnp.concatenate(
        [
            jnp.where(
                lane < head_size,
                stats[:, offset + head : offset + head + 1],
                stats[:, offset + head + 1 : offset + head + 2],
            )
            for head in range(0, heads, 2)
        ],
        axis=1,
    )


def attend_rows(queries, keys, values, adjust, live, heads, head_size, scale):
    props = queries.shape[0]
    quad = 4
    width = quad * head_size
    row_head = lax.broadcasted_iota(jnp.int32, (quad * props, width), 0) // props
    col_head = lax.broadcasted_iota(jnp.int32, (quad * props, width), 1) // head_size
    own = (row_head == col_head).astype(jnp.float32).astype(jnp.bfloat16)
    lane = lax.broadcasted_iota(jnp.int32, (props, LANES), 1)
    tiles, peaks, totals = [], [], []
    for group in range(heads // quad):
        columns = slice(group * width, (group + 1) * width)
        stacked = jnp.concatenate([queries[:, columns]] * quad, axis=0) * own
        scores = lax.dot_general(
            stacked, keys[:, columns], (((1,), (1,)), ((), ())), preferred_element_type=jnp.float32
        )
        weights = []
        for inner in range(quad):
            head = group * quad + inner
            part = scores[inner * props : (inner + 1) * props] * scale - adjust(head)
            part = jnp.where(live, part, MASKED)
            peak = jnp.max(part, axis=1, keepdims=True)
            weight = jnp.where(live, jnp.exp(part - peak), 0.0)
            peaks.append(peak)
            totals.append(jnp.sum(weight, axis=1, keepdims=True))
            weights.append(weight.astype(jnp.bfloat16))
        summed = jnp.dot(
            jnp.concatenate(weights, axis=0), values[:, columns], preferred_element_type=jnp.float32
        )
        for pair in range(quad // 2):
            cols = slice(pair * LANES, (pair + 1) * LANES)
            first = summed[2 * pair * props : (2 * pair + 1) * props, cols]
            second = summed[(2 * pair + 1) * props : (2 * pair + 2) * props, cols]
            tiles.append(jnp.where(lane < head_size, first, second))
    return jnp.concatenate(tiles, axis=1), peaks, totals


def pack_stats(columns, props):
    lane = lax.broadcasted_iota(jnp.int32, (props, LANES), 1)
    stats = jnp.zeros((props, LANES), jnp.float32)
    for index, column in enumerate(columns):
        stats = jnp.where(lane == index, column, stats)
    return stats


def layer_kernel(
    sizes,
    lengths,
    accepted,
    parents,
    tokens,
    norm_gain,
    w_query,
    w_key,
    w_value,
    w_forget,
    forget_bias,
    query_gain,
    key_gain,
    head_gain,
    w_out,
    key_cache,
    value_cache,
    gate_cache,
    out_layer,
    out_rows,
    out_gates,
    kc_v,
    vc_v,
    tok_v,
    norm_v,
    wq_v,
    wk_v,
    wv_v,
    wf_v,
    bias_v,
    qgain_v,
    kgain_v,
    hgain_v,
    wo_v,
    gc_v,
    send_q,
    send_kv,
    got_q,
    got_kv,
    all_q,
    all_gates,
    all_kv,
    send_part,
    got_part,
    send_stats,
    got_stats,
    all_normed,
    term_own,
    term_other,
    load_sem,
    sent_sem,
    came_sem,
    pair_sem,
):
    n, heads, head_size, full_width = sizes
    me = lax.axis_index("kv")
    core = lax.axis_index("tp")
    seqs, props, width_in = tok_v.shape
    head_width = heads * head_size
    pos_dev = kc_v.shape[1]
    rows_all = seqs * props
    scale = head_size ** (-0.5)
    order = sorted(range(1, n), key=lambda step: abs(2 * step - n))

    forget_columns = pl.ds(pl.multiple_of(me * width_in, width_in), width_in)
    loads = {}
    for index, (name, source, target) in enumerate(
        (
            ("tokens", tokens, tok_v),
            ("norm", norm_gain, norm_v),
            ("wq", w_query, wq_v),
            ("wf", w_forget.at[:, forget_columns], wf_v),
            ("bias", forget_bias, bias_v),
            ("qgain", query_gain, qgain_v),
            ("kgain", key_gain, kgain_v),
            ("hgain", head_gain, hgain_v),
            ("wk", w_key, wk_v),
            ("wv", w_value, wv_v),
            ("gates", gate_cache, gc_v),
            ("keys", key_cache, kc_v),
            ("values", value_cache, vc_v),
            ("wo", w_out, wo_v),
        )
    ):
        loads[name] = pltpu.make_async_copy(source, target, load_sem.at[index])
        loads[name].start()

    barrier = pltpu.get_barrier_semaphore()
    for step in order:
        pl.semaphore_signal(
            barrier, inc=1, device_id={"kv": lax.rem(me + step, n)}, device_id_type=MESH
        )
    pl.semaphore_signal(barrier, inc=1, device_id={"tp": 1 - core}, device_id_type=MESH)

    sent = []

    def push(phase, step, source, target):
        peer = lax.rem(me + step, n)
        copy = pltpu.make_async_remote_copy(
            src_ref=source(peer),
            dst_ref=target.at[me],
            send_sem=sent_sem.at[phase, step],
            recv_sem=came_sem.at[phase, me],
            device_id={"kv": peer},
            device_id_type=MESH,
        )
        copy.start()
        sent.append(copy)

    def arrive(phase, step, target):
        peer = lax.rem(me + step, n)
        pltpu.make_async_remote_copy(
            src_ref=target.at[peer],
            dst_ref=target.at[peer],
            send_sem=sent_sem.at[phase, step],
            recv_sem=came_sem.at[phase, peer],
            device_id={"kv": peer},
            device_id_type=MESH,
        ).wait_recv()

    loads["tokens"].wait()
    loads["norm"].wait()
    flat = tok_v[...].astype(jnp.float32).reshape(rows_all, width_in)
    squares = jnp.sum(flat * flat, axis=1, keepdims=True)
    scaled = (flat * norm_v[...]).astype(jnp.bfloat16)
    loads["wq"].wait()
    loads["wf"].wait()
    send_q[:, :, :head_width] = jnp.dot(
        scaled, wq_v[...], preferred_element_type=jnp.float32
    ).reshape(seqs, props, head_width)
    gate_part = lax.dot_general(
        scaled, wf_v[...], (((1,), (1,)), ((), ())), preferred_element_type=jnp.float32
    )
    gate_heads = gate_part.shape[1]
    send_q[:, :, head_width:] = jnp.broadcast_to(squares, (rows_all, LANES)).reshape(
        seqs, props, LANES
    )
    send_q[:, :, head_width : head_width + gate_heads] = gate_part.reshape(seqs, props, gate_heads)
    pl.semaphore_wait(barrier, n)
    for step in order:
        push(0, step, lambda peer: send_q.at[peer], got_q)

    loads["wk"].wait()
    send_kv[:, :, :head_width] = jnp.dot(
        scaled, wk_v[...], preferred_element_type=jnp.float32
    ).reshape(seqs, props, head_width)
    loads["wv"].wait()
    send_kv[:, :, head_width:] = jnp.dot(
        scaled, wv_v[...], preferred_element_type=jnp.float32
    ).reshape(seqs, props, head_width)

    row = lax.broadcasted_iota(jnp.int32, (LANES, LANES), 0)
    column = lax.broadcasted_iota(jnp.int32, (LANES, LANES), 1)
    eye = (row == column).astype(jnp.float32)
    target_column = jnp.full((LANES, LANES), -1, jnp.int32)
    for prop in range(props):
        target_column = jnp.where(row == prop, parents[me, prop], target_column)
    power = (target_column == column).astype(jnp.float32)
    ancestors = eye + power
    reach = 2
    while reach < props:
        half = power.astype(jnp.bfloat16)
        power = jnp.dot(half, half, preferred_element_type=jnp.float32)
        ancestors = ancestors + jnp.dot(
            ancestors.astype(jnp.bfloat16),
            power.astype(jnp.bfloat16),
            preferred_element_type=jnp.float32,
        )
        reach *= 2
    for name in ("bias", "qgain", "kgain", "hgain"):
        loads[name].wait()
    gain_q = jnp.concatenate([qgain_v[...]] * (LANES // head_size), axis=1)
    gain_k = jnp.concatenate([kgain_v[...]] * (LANES // head_size), axis=1)
    gain_h = jnp.concatenate([hgain_v[...]] * (LANES // head_size), axis=1)

    for step in order:
        arrive(0, step, got_q)
    raw = send_q[me]
    for step in range(1, n):
        raw = raw + got_q[lax.rem(me + step, n)]
    small = raw[:, head_width:]
    inverse = lax.rsqrt(small[:, gate_heads : gate_heads + 1] / full_width + EPSILON)
    all_q[me] = tile_head_norm(raw[:, :head_width] * inverse, gain_q, head_size).astype(
        jnp.bfloat16
    )
    for step in order:
        push(1, step, lambda peer: all_q.at[me], all_q)
    logits = small[:, :gate_heads] * inverse + bias_v[...]
    logs = -(jnp.maximum(-logits, 0.0) + jnp.log1p(jnp.exp(-jnp.abs(logits))))
    logs = jnp.where(core == 0, logs[:, :heads], logs[:, heads:])
    side_row = lax.broadcasted_iota(jnp.int32, (props, LANES), 0)
    side_column = lax.broadcasted_iota(jnp.int32, (props, LANES), 1)
    turned = side_row == side_column
    all_gates[me] = jnp.concatenate(
        [
            jnp.sum(jnp.where(turned, logs[:, head : head + 1], 0.0), axis=0, keepdims=True)
            for head in range(heads)
        ],
        axis=0,
    )
    log_wide = pack_stats([logs[:, head : head + 1] for head in range(heads)], props)
    for step in order:
        push(2, step, lambda peer: send_kv.at[peer], got_kv)
    for step in order:
        push(3, step, lambda peer: all_gates.at[me], all_gates)

    lane_pos = me * pos_dev + lax.broadcasted_iota(jnp.int32, (props, pos_dev), 1)
    loads["gates"].wait()
    loads["keys"].wait()
    loads["values"].wait()
    for step in [0] + order:
        seq = lax.rem(me + step, n)
        if step:
            arrive(1, step, all_q)
        base = lengths[seq] + accepted[seq]
        gate_rows = gc_v[seq]
        hit = lane_pos == base - 1
        total, peaks, totals = attend_rows(
            all_q[seq],
            kc_v[seq],
            vc_v[seq],
            lambda head: gate_rows[head : head + 1],
            lane_pos < base,
            heads,
            head_size,
            scale,
        )
        edges = [
            jnp.sum(
                jnp.where(hit[:1], gate_rows[head : head + 1], 0.0), axis=1, keepdims=True
            )
            for head in range(heads)
        ]
        send_part[seq] = total.astype(jnp.bfloat16)
        send_stats[seq] = pack_stats(peaks + totals + edges, props)
        if step:
            push(4, step, lambda peer: send_part.at[peer], got_part)
            push(7, step, lambda peer: send_stats.at[peer], got_stats)
        else:
            own_total = total

    for step in order:
        arrive(2, step, got_kv)
    raw = send_kv[me]
    for step in range(1, n):
        raw = raw + got_kv[lax.rem(me + step, n)]
    raw = raw * inverse
    keys_own = tile_head_norm(raw[:, :head_width], gain_k, head_size).astype(jnp.bfloat16)
    values_own = raw[:, head_width:].astype(jnp.bfloat16)
    all_kv[me, :, :head_width] = keys_own
    all_kv[me, :, head_width:] = values_own
    for step in order:
        push(5, step, lambda peer: all_kv.at[me], all_kv)

    padding = jnp.zeros((LANES - props, head_width), jnp.bfloat16)
    log_tile = jnp.concatenate(
        [log_wide, jnp.zeros((LANES - props, LANES), jnp.float32)], axis=0
    )
    path_sum = jnp.dot(ancestors, log_tile, precision=lax.Precision.HIGHEST)
    on_diagonal = row == column
    tree_sum, tree_peaks, tree_totals = attend_rows(
        all_q[me],
        jnp.concatenate([keys_own, padding], axis=0),
        jnp.concatenate([values_own, padding], axis=0),
        lambda head: jnp.sum(
            jnp.where(on_diagonal, path_sum[:, head : head + 1], 0.0), axis=0, keepdims=True
        ),
        ancestors[:props] > 0.5,
        heads,
        head_size,
        scale,
    )
    tree_stats = pack_stats(tree_peaks + tree_totals, props)

    for step in order:
        arrive(4, step, got_part)
        arrive(7, step, got_stats)
    peers = [lax.rem(me + step, n) for step in range(1, n)]
    stats = [send_stats[me]] + [got_stats[peer] for peer in peers]
    edge = functools.reduce(jnp.add, stats)
    tops = [spread_heads(each, 0, heads, head_size) for each in stats]
    sums = [spread_heads(each, heads, heads, head_size) for each in stats]
    numbers = [own_total] + [got_part[peer].astype(jnp.float32) for peer in peers]
    tops.append(
        spread_heads(tree_stats, 0, heads, head_size)
        - spread_heads(edge, 2 * heads, heads, head_size)
    )
    sums.append(spread_heads(tree_stats, heads, heads, head_size))
    numbers.append(tree_sum)
    top = functools.reduce(jnp.maximum, tops)
    factors = [jnp.exp(each - top) for each in tops]
    weighted = functools.reduce(jnp.add, [x * y for x, y in zip(numbers, factors)])
    row_total = functools.reduce(jnp.add, [x * y for x, y in zip(sums, factors)])
    all_normed[me] = tile_head_norm(weighted / row_total, gain_h, head_size).astype(jnp.bfloat16)
    for step in order:
        push(6, step, lambda peer: all_normed.at[me], all_normed)
    loads["wo"].wait()
    for step in order:
        arrive(6, step, all_normed)
    term_own[...] = jnp.dot(
        all_normed[...].reshape(rows_all, head_width),
        wo_v[...],
        preferred_element_type=jnp.float32,
    ).astype(jnp.bfloat16)
    pair = pltpu.make_async_remote_copy(
        src_ref=term_own,
        dst_ref=term_other,
        send_sem=pair_sem.at[0],
        recv_sem=pair_sem.at[1],
        device_id={"tp": 1 - core},
        device_id_type=MESH,
    )
    pair.start()
    for step in order:
        arrive(3, step, all_gates)
    for step in order:
        arrive(5, step, all_kv)
    out_gates[...] = all_gates[:, :, :props]
    out_rows[...] = all_kv[...]
    pair.wait()
    joined = term_own[...].astype(jnp.float32) + term_other[...].astype(jnp.float32)
    out_layer[...] = joined.astype(jnp.bfloat16).reshape(out_layer.shape)
    for copy in sent:
        copy.wait_send()


def write_kernel(
    lengths,
    accepted,
    layer_in,
    rows_in,
    gates_in,
    key_cache,
    value_cache,
    layer_out,
    new_keys,
    new_values,
    gates_out,
    windows,
    in_sem,
    out_sem,
):
    seqs, pos_dev, head_width = key_cache.shape
    props = rows_in.shape[1]
    window = 2 * props
    start = lax.axis_index("kv") * pos_dev
    caches = ((key_cache, new_keys), (value_cache, new_values))
    bulk = [
        [
            pltpu.make_async_copy(held.at[seq], target.at[seq], in_sem.at[side, seq])
            for side, (held, target) in enumerate(caches)
        ]
        for seq in range(seqs)
    ]
    for pair in bulk:
        for copy in pair:
            copy.start()
    layer_out[...] = layer_in[...]
    gates_out[...] = gates_in[...]
    slot = lax.broadcasted_iota(jnp.int32, (window, props), 0)
    prop = lax.broadcasted_iota(jnp.int32, (window, props), 1)
    line = lax.broadcasted_iota(jnp.int32, (window, head_width), 0)
    patches = []
    for seq in range(seqs):
        offset = lengths[seq] + accepted[seq] - start
        inside = jnp.clip(offset, 0, pos_dev - 1)
        lower = jnp.minimum(inside // props * props, pos_dev - window)
        rows = pl.ds(pl.multiple_of(lower, props), window)
        placing = (slot + lower - offset == prop).astype(jnp.float32).astype(jnp.bfloat16)
        place = line + lower - offset
        hit = (place >= 0) & (place < props)
        for side, (held, target) in enumerate(caches):
            fresh = jnp.dot(
                placing,
                rows_in[seq, :, side * head_width : (side + 1) * head_width],
                preferred_element_type=jnp.float32,
            )
            kept = held[seq, rows, :].astype(jnp.float32)
            windows[side, seq] = jnp.where(hit, fresh, kept).astype(jnp.bfloat16)
            patches.append(
                pltpu.make_async_copy(
                    windows.at[side, seq], target.at[seq, rows, :], out_sem.at[side, seq]
                )
            )
    for seq in range(seqs):
        for side in range(2):
            bulk[seq][side].wait()
            patches[2 * seq + side].start()
    for copy in patches:
        copy.wait()


def fused_shards(
    tokens,
    norm_gain,
    w_query,
    w_key,
    w_value,
    w_forget,
    forget_bias,
    query_gain,
    key_gain,
    head_gain,
    w_out,
    key_cache,
    value_cache,
    gate_cache,
    lengths,
    accepted,
    parents,
    n,
):
    seqs, props, width_in = tokens.shape
    pos_dev, head_width = key_cache.shape[1:]
    heads = gate_cache.shape[1]
    head_size = head_width // heads
    width_out = w_out.shape[1]
    bf16, f32 = jnp.bfloat16, jnp.float32
    smem = pl.BlockSpec(memory_space=pltpu.SMEM)
    vmem = pl.BlockSpec(memory_space=pltpu.VMEM)
    any_space = pl.BlockSpec(memory_space=pltpu.HBM)
    line = lambda vector: vector.reshape(1, -1)
    operands = (
        tokens,
        line(norm_gain),
        w_query,
        w_key,
        w_value,
        w_forget.T,
        line(forget_bias),
        line(query_gain),
        line(key_gain),
        line(head_gain),
        w_out,
        key_cache,
        value_cache,
        gate_cache,
    )
    part_width = head_width + LANES
    scratch = [
        pltpu.VMEM(tokens.shape, bf16),
        pltpu.VMEM((1, width_in), f32),
        pltpu.VMEM(w_query.shape, bf16),
        pltpu.VMEM(w_key.shape, bf16),
        pltpu.VMEM(w_value.shape, bf16),
        pltpu.VMEM((w_forget.shape[1], width_in), bf16),
        pltpu.VMEM((1, forget_bias.shape[0]), f32),
        pltpu.VMEM((1, head_size), f32),
        pltpu.VMEM((1, head_size), f32),
        pltpu.VMEM((1, head_size), f32),
        pltpu.VMEM(w_out.shape, bf16),
        pltpu.VMEM(gate_cache.shape, f32),
        pltpu.VMEM((seqs, props, part_width), f32),
        pltpu.VMEM((seqs, props, 2 * head_width), f32),
        pltpu.VMEM((n, props, part_width), f32),
        pltpu.VMEM((n, props, 2 * head_width), f32),
        pltpu.VMEM((n, props, head_width), bf16),
        pltpu.VMEM((n, heads, LANES), f32),
        pltpu.VMEM((n, props, 2 * head_width), bf16),
        pltpu.VMEM((seqs, props, head_width), bf16),
        pltpu.VMEM((n, props, head_width), bf16),
        pltpu.VMEM((seqs, props, LANES), f32),
        pltpu.VMEM((n, props, LANES), f32),
        pltpu.VMEM((n, props, head_width), bf16),
        pltpu.VMEM((seqs * props, width_out), bf16),
        pltpu.VMEM((seqs * props, width_out), bf16),
        pltpu.SemaphoreType.DMA((14,)),
        pltpu.SemaphoreType.DMA((8, n)),
        pltpu.SemaphoreType.DMA((8, n)),
        pltpu.SemaphoreType.DMA((2,)),
    ]
    layer, rows, gates, *held = pl.pallas_call(
        functools.partial(layer_kernel, (n, heads, head_size, w_forget.shape[0])),
        out_shape=(
            pltpu.VMEM((seqs, props, width_out), bf16),
            pltpu.VMEM((seqs, props, 2 * head_width), bf16),
            pltpu.VMEM((seqs, heads, props), f32),
            pltpu.VMEM(key_cache.shape, bf16),
            pltpu.VMEM(value_cache.shape, bf16),
        ),
        in_specs=[smem] * 3 + [any_space] * len(operands),
        out_specs=(vmem,) * 5,
        scratch_shapes=scratch,
        compiler_params=pltpu.CompilerParams(
            collective_id=0, has_side_effects=True, vmem_limit_bytes=62586880
        ),
        name="layer",
    )(lengths, accepted, parents, *operands)
    layer, new_keys, new_values, gates = pl.pallas_call(
        write_kernel,
        out_shape=(
            jax.ShapeDtypeStruct(layer.shape, bf16),
            jax.ShapeDtypeStruct(key_cache.shape, bf16),
            jax.ShapeDtypeStruct(value_cache.shape, bf16),
            jax.ShapeDtypeStruct(gates.shape, f32),
        ),
        in_specs=[smem, smem] + [vmem] * 5,
        out_specs=(vmem, any_space, any_space, vmem),
        scratch_shapes=[
            pltpu.VMEM((2, seqs, 2 * props, head_width), bf16),
            pltpu.SemaphoreType.DMA((2, seqs)),
            pltpu.SemaphoreType.DMA((2, seqs)),
        ],
        compiler_params=pltpu.CompilerParams(vmem_limit_bytes=16 << 20),
        name="write",
    )(lengths, accepted, layer, rows, gates, *held)
    return layer, new_keys, new_values, jnp.swapaxes(gates, 1, 2)


def pick_shards(n, cores):
    def chosen(*arrays):
        tokens, key_cache, gate_cache = arrays[0], arrays[11], arrays[13]
        heads = gate_cache.shape[1]
        fits = (
            tokens.shape[0] == n
            and n > 1
            and cores == 2
            and tokens.shape[1] == 16
            and tokens.shape[2] % LANES == 0
            and key_cache.shape[2] == 64 * heads
            and heads % 4 == 0
            and 3 * heads <= LANES
        )
        return fused_shards(*arrays, n) if fits else shards(*arrays)

    return chosen


def solution(mesh):
    placed = (
        P("dp", None, "kv"),
        P("kv"),
        P("kv", "tp"),
        P("kv", "tp"),
        P("kv", "tp"),
        P(),
        P(),
        P(),
        P(),
        P(),
        P("tp", "kv"),
        P("dp", "kv", "tp"),
        P("dp", "kv", "tp"),
        P("dp", "tp", "kv"),
        P("dp"),
        P("dp"),
        P("dp", None),
    )
    return jax.shard_map(
        pick_shards(mesh.shape["kv"], mesh.shape["tp"]),
        mesh=mesh,
        in_specs=placed,
        out_specs=(
            P("dp", None, "kv"),
            P("dp", "kv", "tp"),
            P("dp", "kv", "tp"),
            P("dp", None, "tp"),
        ),
        check_vma=False,
    )
```
